128 devices in a mesh: sp: 16 (over z, y), fs: 4 (over x), tp: 2 (over core).
Axes of the slice: x: 4, y: 4, z: 4, core: 2. Of those that a mesh axis runs over, the one named last changes fastest.
Arguments:
- attn_query: bfloat16 [4, 4096, 2048], P('fs', 'sp', 'tp'), may hold values from -8 to 8
- attn_key: bfloat16 [4, 4096, 2048], P('fs', 'sp', 'tp'), may hold values from -8 to 8
- attn_value: bfloat16 [4, 4096, 2048], P('fs', 'sp', 'tp'), may hold values from -6 to 6
- head_lambda: float32 [16], P('tp'), may hold values from 0.3 to 0.8
- cell_query: bfloat16 [4, 4096, 1024], P('fs', 'sp', 'tp'), may hold values from -6 to 6
- cell_key: bfloat16 [4, 4096, 1024], P('fs', 'sp', 'tp'), may hold values from -6 to 6
- cell_value: bfloat16 [4, 4096, 2048], P('fs', 'sp', 'tp'), may hold values from -6 to 6
- input_pre: float32 [4, 16, 4096], P('fs', 'tp', 'sp'), may hold values from -5 to 140
- forget_pre: float32 [4, 16, 4096], P('fs', 'tp', 'sp'), may hold values from -2 to 16
- out_attn: bfloat16 [2048, 2048], P('tp', 'fs'), may hold values from -0.09375 to 0.09375
- out_cell: bfloat16 [2048, 2048], P('tp', 'fs'), may hold values from -0.09375 to 0.09375
Outputs:
- layer_out: bfloat16 [4, 4096, 2048], P('fs', ('sp', 'tp'))
The draws below stay inside these ranges and needn't reach their ends.
All inputs are finite; a program needn't handle non-finite values.
Results may differ from the reference program's by a relative error of at most 0.0095.
Values may be sent and summed in bfloat16 or wider, within the bound.
A program may use at most 128 MiB of HBM per device.

```python
import math
import jax
import jax.numpy as jnp
from jax import lax

D = 2048
HA = 16
DK = 64
DV = 128
HC = 16
CK = 64
CV = 128
TOK_DEV = 256
LENGTH = 4096
SEQS = 4
N_TP = 2


def attention_pair(key):
    shape = (SEQS, LENGTH, HA * 2 * DK)
    query = jnp.clip(1.32 * jax.random.normal(jax.random.fold_in(key, 11), shape, jnp.float32), -8.0, 8.0)
    keyed = jnp.clip(1.32 * jax.random.normal(jax.random.fold_in(key, 12), shape, jnp.float32), -8.0, 8.0)
    return (query, keyed)


def draw_attn_query(key, part):
    return attention_pair(key)[0].astype(jnp.bfloat16)


def draw_attn_key(key, part):
    return attention_pair(key)[1].astype(jnp.bfloat16)


def draw_input_pre(key, part):
    shape = (SEQS, HC, LENGTH)
    value_rows = jnp.clip(jax.random.normal(jax.random.fold_in(key, 31), shape, jnp.float32), -5.0, 5.0)
    return value_rows


def draw_forget_pre(key, part):
    shape = (SEQS, HC, LENGTH)
    slow_share = 0.5
    jitter = jnp.clip(0.7 * jax.random.normal(jax.random.fold_in(key, 42), shape, jnp.float32), -2.0, 2.0)
    slow = jax.random.uniform(jax.random.fold_in(key, 41), (SEQS, HC, 1)) < slow_share
    rate = jnp.where(slow, 0.5 / LENGTH, 0.02)
    base = -jnp.log(jnp.expm1(rate))
    offsets = jax.random.uniform(jax.random.fold_in(key, 43), (SEQS, HC, LENGTH // TOK_DEV), jnp.float32, -0.7, 0.7)
    offsets = jnp.repeat(offsets, TOK_DEV, axis=2)
    value_rows = base + jitter + offsets
    chosen_locations = jax.random.randint(jax.random.fold_in(key, 44), (SEQS, 1, 3), 0, LENGTH)
    retained_rows = jax.random.uniform(jax.random.fold_in(key, 45), (SEQS, HC, 3), jnp.float32, 0.5, 0.8)
    spike_value_level = -jnp.log(1.0 / retained_rows - 1.0)
    target_locations = jnp.arange(LENGTH)[None, None, :]
    for lookup_index in range(3):
        value_rows = jnp.where(target_locations == chosen_locations[:, :, lookup_index:lookup_index + 1], spike_value_level[:, :, lookup_index:lookup_index + 1], value_rows)
    return value_rows


def block_scale(rng, dims, shards, smallest, high):
    factor_of = 1.0
    for position, shards_of in shards:
        steps = jax.random.uniform(jax.random.fold_in(jax.random.fold_in(rng, 6), position), (shards_of,), jnp.float32, smallest / len(shards), high / len(shards))
        factor_of = factor_of * jnp.repeat(jnp.exp(steps), dims[position] // shards_of).reshape((-1,) + (1,) * (len(dims) - 1 - position))
    return factor_of


def noise(stream_key, dims, deviation, bound, cuts=(), kind=jnp.bfloat16):
    array = deviation * jax.random.normal(stream_key, dims, jnp.float32)
    if cuts:
        array = array * block_scale(stream_key, dims, cuts, -0.22, 0.18)
    return jnp.clip(array, -bound, bound).astype(kind)


def setup_inputs(seed: int = 0) -> dict:
    seeds = jax.random.split(jax.random.key(seed), 12)
    return {
        "attn_query": draw_attn_query(jax.random.fold_in(seeds[11], 71), 0),
        "attn_key": draw_attn_key(jax.random.fold_in(seeds[11], 71), 0),
        "attn_value": noise(seeds[2], (SEQS, LENGTH, HA * DV), 1.0, 6.0, ((0, 4), (1, 16), (2, 2))),
        "head_lambda": jnp.clip(0.3 + 0.5 * jax.random.uniform(seeds[3], (HA,), jnp.float32) ** block_scale(seeds[3], (HA,), ((0, 2),), -0.2, 0.2), 0.3, 0.8),
        "cell_query": noise(seeds[4], (SEQS, LENGTH, HC * CK), 1.0, 6.0, ((0, 4), (1, 16), (2, 2))),
        "cell_key": noise(seeds[5], (SEQS, LENGTH, HC * CK), 1.0, 6.0, ((0, 4), (1, 16), (2, 2))),
        "cell_value": noise(seeds[6], (SEQS, LENGTH, HC * CV), 1.0, 6.0, ((0, 4), (1, 16), (2, 2))),
        "input_pre": draw_input_pre(jax.random.fold_in(seeds[11], 71), 0),
        "forget_pre": draw_forget_pre(jax.random.fold_in(seeds[11], 71), 0),
        "out_attn": noise(seeds[9], (HA * DV, D), (HA * DV + HC * CV) ** -0.5, 0.09375, ((0, 2), (1, 4))),
        "out_cell": noise(seeds[10], (HC * CV, D), (HA * DV + HC * CV) ** -0.5, 0.09375, ((0, 2), (1, 4))),
    }


EPS = 1e-06
LAMBDA_INIT = 0.2
NEG = -1e+30

def head_norm(value_rows, heads):
    rows = value_rows.shape[0]
    grouped = value_rows.reshape(rows, heads, -1)
    factor = lax.rsqrt(lax.optimization_barrier(jnp.mean(grouped * grouped, axis=-1, keepdims=True)) + EPS)
    return (grouped * factor).reshape(rows, -1)

def attention_one(query, keyed, valued, head_lambda):
    length = query.shape[0]
    queries = query.reshape(length, HA, 2, DK).astype(jnp.float32)
    keys_all = keyed.reshape(length, HA, 2, DK).astype(jnp.float32)
    values_all = valued.reshape(length, HA, DV).astype(jnp.float32)
    block = math.gcd(length, 128)
    positions = jnp.arange(length, dtype=jnp.int32)

    def one_block(first):
        rows = lax.dynamic_slice_in_dim(queries, first, block, 0)
        scores = jnp.einsum('qhcd,khcd->hcqk', rows, keys_all) * DK ** (-0.5)
        row_pos = first + jnp.arange(block, dtype=jnp.int32)
        scores = jnp.where(positions[None, :] <= row_pos[:, None], scores, NEG)
        row_max = lax.optimization_barrier(jnp.max(scores, axis=-1, keepdims=True))
        expd = jnp.exp(scores - row_max)
        row_total = lax.optimization_barrier(jnp.sum(expd, axis=-1))
        rounded = lax.optimization_barrier(expd.astype(jnp.bfloat16)).astype(jnp.float32)
        ratio = jnp.einsum('hcqk,khd->hcqd', rounded, values_all) / row_total[..., None]
        mixed = ratio[:, 0] - head_lambda[:, None, None] * ratio[:, 1]
        return jnp.transpose(mixed, (1, 0, 2))
    firsts = jnp.arange(0, length, block, dtype=jnp.int32)
    mixed = lax.map(one_block, firsts).reshape(length, HA * DV)
    return (head_norm(mixed, HA) * (1.0 - LAMBDA_INIT)).astype(jnp.bfloat16)

def cell_summary(keys_blk, values_blk, gate_blk, forget_blk):
    cumul = jnp.cumsum(forget_blk, axis=-1)
    totals = cumul[:, -1]
    expo = totals[:, None] - cumul + gate_blk
    local_max = lax.optimization_barrier(jnp.max(expo, axis=-1))
    scaled = jnp.exp(expo - local_max[:, None])
    weighted = (scaled[:, :, None] * keys_blk.astype(jnp.float32)).astype(jnp.bfloat16)
    weighted = lax.optimization_barrier(weighted).astype(jnp.float32)
    local_state = jnp.einsum('htd,hte->hde', weighted, values_blk.astype(jnp.float32))
    return (cumul, totals, local_max, local_state)

def cell_output(query_blk, keys_blk, values_blk, gate_blk, cumul, prev_state, prior_stabilizer):
    length = cumul.shape[-1]
    diff = cumul[:, :, None] - cumul[:, None, :] + gate_blk[:, None, :]
    causal = jnp.arange(length, dtype=jnp.int32)[:, None] >= jnp.arange(length, dtype=jnp.int32)[None, :]
    diff = jnp.where(causal[None], diff, NEG)
    inter = cumul + prior_stabilizer[:, None]
    stab = jnp.maximum(lax.optimization_barrier(jnp.max(diff, axis=-1)), inter)
    query_f = query_blk.astype(jnp.float32)
    scores = jnp.einsum('hjd,hkd->hjk', query_f, keys_blk.astype(jnp.float32)) * CK ** (-0.5)
    probs = (jnp.exp(diff - stab[..., None]) * scores).astype(jnp.bfloat16)
    probs = lax.optimization_barrier(probs).astype(jnp.float32)
    intra = jnp.einsum('hjk,hke->hje', probs, values_blk.astype(jnp.float32))
    carried = jnp.einsum('hjd,hde->hje', query_f, prev_state, precision=lax.Precision.HIGHEST) * CK ** (-0.5)
    return intra + jnp.exp(inter - stab)[..., None] * carried

def cell_one(query, keyed, valued, in_gate, forget):
    length = query.shape[0]
    blocks = length // TOK_DEV
    queries = query.reshape(blocks, TOK_DEV, HC, CK).transpose(0, 2, 1, 3)
    keys_all = keyed.reshape(blocks, TOK_DEV, HC, CK).transpose(0, 2, 1, 3)
    values_all = valued.reshape(blocks, TOK_DEV, HC, CV).transpose(0, 2, 1, 3)
    gates = in_gate.reshape(HC, blocks, TOK_DEV).transpose(1, 0, 2)
    forgets = jax.nn.log_sigmoid(forget.reshape(HC, blocks, TOK_DEV).transpose(1, 0, 2))

    def advance(carry, pieces):
        prev_state, prior_stabilizer = carry
        query_blk, keys_blk, values_blk, gate_blk, forget_blk = pieces
        cumul, totals, local_max, local_state = cell_summary(keys_blk, values_blk, gate_blk, forget_blk)
        hidden = cell_output(query_blk, keys_blk, values_blk, gate_blk, cumul, prev_state, prior_stabilizer)
        new_stab = jnp.maximum(totals + prior_stabilizer, local_max)
        new_state = jnp.exp(totals + prior_stabilizer - new_stab)[:, None, None] * prev_state + jnp.exp(local_max - new_stab)[:, None, None] * local_state
        return ((new_state, new_stab), hidden)
    start = (jnp.zeros((HC, CK, CV), jnp.float32), jnp.zeros((HC,), jnp.float32))
    _, hidden = lax.scan(advance, start, (queries, keys_all, values_all, gates, forgets))
    hidden = hidden.transpose(0, 2, 1, 3).reshape(length, HC * CV)
    return head_norm(hidden, HC).astype(jnp.bfloat16)

def project(attn_out, cell_out, out_attn, out_cell):
    rows_attn = HA * DV // N_TP
    rows_cell = HC * CV // N_TP
    summed = jnp.zeros((attn_out.shape[0], D), jnp.float32)
    for group in range(N_TP):
        part = jnp.dot(attn_out[:, group * rows_attn:(group + 1) * rows_attn], out_attn[group * rows_attn:(group + 1) * rows_attn], preferred_element_type=jnp.float32)
        part = part + jnp.dot(cell_out[:, group * rows_cell:(group + 1) * rows_cell], out_cell[group * rows_cell:(group + 1) * rows_cell], preferred_element_type=jnp.float32)
        summed = summed + lax.optimization_barrier(part.astype(jnp.bfloat16)).astype(jnp.float32)
    return summed.astype(jnp.bfloat16)

def reference(attn_query, attn_key, attn_value, head_lambda, cell_query, cell_key, cell_value, input_pre, forget_pre, out_attn, out_cell):
    results = []
    for sequence in range(SEQS):
        attn_out = attention_one(attn_query[sequence], attn_key[sequence], attn_value[sequence], head_lambda)
        cell_out = cell_one(cell_query[sequence], cell_key[sequence], cell_value[sequence], input_pre[sequence], forget_pre[sequence])
        results.append(project(attn_out, cell_out, out_attn, out_cell))
    return jnp.stack(results)
```

```python
import functools

import jax
import jax.numpy as jnp
from jax import lax
from jax.experimental import pallas as pl
from jax.experimental.pallas import tpu as pltpu
from jax.sharding import PartitionSpec as P

MESH = pl.DeviceIdType.MESH
F32 = jnp.float32
BF16 = jnp.bfloat16
NEG = -1e30
EPS = 1e-6

TOK = 256
NSP = 16
NFS = 4
HEADS = 8
DV = 128


def dot_nn(a, b):
    return jnp.dot(a, b, preferred_element_type=F32)


def dot_nt(a, b):
    return lax.dot_general(a, b, (((1,), (1,)), ((), ())), preferred_element_type=F32)


def iota(shape, dim):
    return lax.broadcasted_iota(jnp.int32, shape, dim)


def log_sigmoid(x):
    small = jnp.exp(-jnp.abs(x))
    series = small * (1.0 - small * (0.5 - small * (1.0 / 3.0 - small * 0.25)))
    return jnp.minimum(x, 0.0) - jnp.where(small < 0.01, series, jnp.log(1.0 + small))


def scan_lanes(x, combine, start):
    lane = iota(x.shape, 1)
    shift = 1
    while shift < x.shape[1]:
        moved = pltpu.roll(x, shift, 1)
        x = combine(x, jnp.where(lane >= shift, moved, start))
        shift *= 2
    return x


def kernel(
    aq, ak, av, lam, cq, ck, cv, gi, gf, wa, wc, out,
    kb, vb, vt, qb, sbuf, mx, ls, acc, aout, acta, actc, w, part, own, got,
    cqs, cks, cvs, intra, cvt, hdr, st_out, st_in, pv_out, pv_in, cum_s, u_s, m_s, lamt,
    k_s, v_s, q_s, k_r, v_r, q_r, rk_s, rv_s, as_, ar, w_s, w_r, p_s, p_r,
    st_s, st_r, pv_s, pv_r, c_r, l_s, l_r,
):
    p = lax.axis_index("sp")
    f = lax.axis_index("fs")
    t = lax.axis_index("tp")
    left, right, across = lax.rem(f + 3, NFS), lax.rem(f + 1, NFS), lax.rem(f + 2, NFS)
    owner = lax.rem((p + 1) // 2, 2)
    group = p // HEADS
    row = lax.rem(p, HEADS)

    def remote(src, dst, send, recv, device):
        return pltpu.make_async_remote_copy(
            src_ref=src, dst_ref=dst, send_sem=send, recv_sem=recv, device_id=device, device_id_type=MESH
        )

    def arrived(dst, recv):
        remote(dst, dst, recv, recv, (p, f, 1 - t)).wait_recv()

    def sent(src, send):
        remote(src, src, send, send, (p, f, 1 - t)).wait_send()

    def kv_at(ref, b):
        return ref.at[b // 2, pl.ds(pl.multiple_of(lax.rem(b, 2) * TOK, TOK), TOK), :]

    def cols(i):
        return pl.ds(pl.multiple_of(i * 128, 128), 128)

    barrier = pltpu.get_barrier_semaphore()

    def greet(i, _):
        peer = lax.rem(p * 2 + t + i, 2 * NSP)
        pl.semaphore_signal(barrier, inc=1, device_id=(peer // 2, f, lax.rem(peer, 2)), device_id_type=MESH)
        return 0

    lax.fori_loop(1, 2 * NSP, greet, 0)
    for side in (left, right):
        pl.semaphore_signal(barrier, inc=1, device_id=(p, side, t), device_id_type=MESH)
    pl.semaphore_wait(barrier, 2 * NSP + 1)

    locals_ = (
        (cq, cqs, c_r.at[0]), (ck, cks, c_r.at[1]), (cv, cvs, c_r.at[2]),
        (wa, w.at[f, 0], w_r.at[0, 0]), (wc, w.at[f, 1], w_r.at[0, 1]),
    )
    for src, dst, sem in locals_:
        pltpu.make_async_copy(src, dst, sem).start()

    def send_heads(i, _):
        j = lax.rem(row + i, HEADS)
        h = HEADS * t + j
        here = jnp.logical_and(h == p, t == owner)
        trips = (
            (ak, kv_at(kb, p), k_s, k_r.at[p]),
            (av, kv_at(vb, p), v_s, v_r.at[p]),
            (aq, qb.at[p // 2], q_s, q_r.at[p // 2]),
        )
        for src, dst, send, recv in trips:

            @pl.when(jnp.logical_not(here))
            def _():
                remote(src.at[:, cols(j)], dst, send.at[j], recv, (h, f, owner)).start()

            @pl.when(here)
            def _():
                pltpu.make_async_copy(src.at[:, cols(j)], dst, recv).start()

        return 0

    lax.fori_loop(0, HEADS, send_heads, 0)

    to_right = [remote(x, w.at[f, i], w_s.at[i], w_r.at[1, i], (p, right, t)) for i, x in enumerate((wa, wc))]
    to_left = [remote(x, w.at[f, i], w_s.at[2 + i], w_r.at[2, i], (p, left, t)) for i, x in enumerate((wa, wc))]
    for copy in (to_right[0], to_left[1], to_right[1], to_left[0]):
        copy.start()

    for i in range(HEADS):
        lamt[t, pl.ds(i, 1), :] = jnp.full((1, TOK), lam[i], F32)
    lam_copy = remote(lamt.at[t], lamt.at[t], l_s, l_r, (p, f, 1 - t))
    lam_copy.start()

    cum = scan_lanes(log_sigmoid(gf[...]), jnp.add, 0.0)
    u = gi[...] - cum
    run = scan_lanes(u, jnp.maximum, NEG)
    cum_s[...] = cum
    u_s[...] = u
    m_s[...] = run
    half = iota((1, 128), 1) < 64
    decay = jnp.broadcast_to(cum[:, TOK - 1 : TOK], (HEADS, 128))
    largest = decay + run[:, TOK - 1 : TOK]
    for k in range(4):
        hdr[k : k + 1, :] = jnp.where(half, decay[2 * k : 2 * k + 1], decay[2 * k + 1 : 2 * k + 2])
        hdr[4 + k : 5 + k, :] = jnp.where(half, largest[2 * k : 2 * k + 1], largest[2 * k + 1 : 2 * k + 2])
    st_out[:, 0:8, :] = jnp.broadcast_to(hdr[...][None], (NSP, 8, 128))
    for src, dst, sem in locals_[:3]:
        pltpu.make_async_copy(src, dst, sem).wait()

    def down(h):
        return jnp.transpose(jnp.broadcast_to(u_s[pl.ds(h, 1), :], (128, TOK)))

    def q_half(pair, which):
        q = cqs[:, cols(pair)] * jnp.asarray(0.125, BF16)
        lane = iota((TOK, 128), 1)
        keep = lane < 64 if which == 0 else lane >= 64
        return jnp.where(keep, q, jnp.zeros_like(q))

    def cell_state(k, _):
        expo = []
        for i in range(2):
            h = 2 * k + i
            expo.append(down(h) - m_s[pl.ds(h, 1), :][:, TOK - 1 : TOK])
            cvt[h] = jnp.transpose(cvs[:, cols(h)].astype(F32)).astype(BF16)
        scaled = jnp.exp(jnp.where(half, expo[0], expo[1]))
        weighted = (scaled * cks[:, cols(k)].astype(F32)).astype(BF16)
        state = jnp.where(half, dot_nn(cvt[2 * k], weighted), dot_nn(cvt[2 * k + 1], weighted))
        st_out[:, pl.ds(pl.multiple_of(8 + 8 * k, 8), 8), :] = state.reshape(NSP, 8, 128)
        return 0

    lax.fori_loop(0, 4, cell_state, 0)

    def send_state(i, _):
        to = lax.rem(p + i, NSP)
        remote(st_out.at[to], st_in.at[p], st_s.at[to], st_r.at[p], (to, f, t)).start()
        return 0

    lax.fori_loop(1, NSP, send_state, 0)
    st_in[p] = st_out[p]

    def cell_inside(k, _):
        keys = cks[:, cols(k)]
        causal = iota((TOK, TOK), 0) <= iota((TOK, TOK), 1)
        for i in range(2):
            h = 2 * k + i
            scores = dot_nt(keys, q_half(k, i))
            rows = down(h)
            diff = jnp.concatenate([rows, rows], axis=1) - m_s[pl.ds(h, 1), :]
            weight = (jnp.exp(jnp.where(causal, diff, NEG)) * scores).astype(BF16)
            intra[h] = dot_nn(cvt[h], weight)
        return 0

    lax.fori_loop(0, 4, cell_inside, 0)

    def wait_state(i, _):
        b = lax.rem(p + i, NSP)
        arrived(st_in.at[b], st_r.at[b])
        return 0

    lax.fori_loop(1, NSP, wait_state, 0)

    def advance(b, carry):
        stab, states = carry
        pv_out[b, 0:4, :] = stab
        decays, tops = st_in[b, 0:4, :], st_in[b, 4:8, :]
        new = jnp.maximum(decays + stab, tops)
        keep, take = jnp.exp(decays + stab - new), jnp.exp(tops - new)
        after = []
        for k in range(4):
            at = slice(8 + 8 * k, 16 + 8 * k)
            pv_out[b, at, :] = states[k]
            after.append(keep[k : k + 1] * states[k] + take[k : k + 1] * st_in[b, at, :])
        return new, tuple(after)

    zero = jnp.zeros((8, 128), F32)
    pv_out[:, 4:8, :] = jnp.zeros((NSP, 4, 128), F32)
    lax.fori_loop(0, NSP, advance, (jnp.zeros((4, 128), F32), (zero,) * 4))

    def send_prev(i, _):
        to = lax.rem(p + i, NSP)
        remote(pv_out.at[to], pv_in.at[p], pv_s.at[to], pv_r.at[p], (to, f, t)).start()
        return 0

    lax.fori_loop(1, NSP, send_prev, 0)
    pv_in[p] = pv_out[p]

    arrived(lamt.at[1 - t], l_r)

    def attend(s, _):
        mine = 2 * s + lax.rem(s + t, 2)
        other = 2 * s + lax.rem(s + t + 1, 2)
        for ref, recv, send in ((kb, k_r, rk_s), (vb, v_r, rv_s)):
            block = kv_at(ref, mine)
            arrived(block, recv.at[mine])
            remote(block, block, send.at[s], recv.at[mine], (p, f, 1 - t)).start()
        arrived(qb.at[s], q_r.at[s])
        for ref, recv in ((kb, k_r), (vb, v_r)):
            arrived(kv_at(ref, other), recv.at[other])
        vt[s] = jnp.transpose(vb[s].astype(F32)).astype(BF16)
        q = qb[s] * jnp.asarray(0.125, BF16)
        lane = iota((TOK, 128), 1)
        none = jnp.zeros_like(q)
        maps = (jnp.where(lane < 64, q, none), jnp.where(lane >= 64, q, none))
        mx[...] = jnp.full(mx.shape, NEG, F32)

        def score(kt, masked):
            keys = kb[kt]
            for c in range(2):
                sc = dot_nt(keys, maps[c])
                if masked:
                    seen = iota(sc.shape, 0) <= iota(sc.shape, 1) + (mine - 2 * s) * TOK
                    sc = jnp.where(seen, sc, NEG)
                sbuf[c, kt] = sc
                mx[c] = jnp.maximum(mx[c], jnp.max(sc.reshape(64, 8, TOK), axis=0))

        def score_one(kt, _):
            score(kt, False)
            return 0

        lax.fori_loop(0, s, score_one, 0)
        score(s, True)
        tops = [jnp.max(mx[c], axis=0, keepdims=True) for c in range(2)]
        ls[...] = jnp.zeros(ls.shape, F32)
        acc[...] = jnp.zeros(acc.shape, F32)

        def weigh(kt, _):
            for c in range(2):
                expd = jnp.exp(sbuf[c, kt] - tops[c])
                ls[c] += jnp.sum(expd.reshape(64, 8, TOK), axis=0)
                acc[c] += dot_nn(vt[kt], expd.astype(BF16))
            return 0

        lax.fori_loop(0, s + 1, weigh, 0)
        ratio = [acc[c] / jnp.sum(ls[c], axis=0, keepdims=True) for c in range(2)]
        mixed = ratio[0] - lamt[group, pl.ds(row, 1), :] * ratio[1]
        factor = lax.rsqrt(jnp.mean(mixed * mixed, axis=0, keepdims=True) + EPS) * 0.8
        aout[s] = jnp.transpose(mixed * factor).astype(BF16)
        home = jnp.logical_and(mine == p, group == t)

        @pl.when(jnp.logical_not(home))
        def _():
            remote(aout.at[s], acta.at[:, cols(row)], as_.at[s], ar.at[row], (mine, f, group)).start()

        @pl.when(home)
        def _():
            acta[:, cols(row)] = aout[s]

        return 0

    lax.fori_loop(0, HEADS, attend, 0)

    arrived(w.at[left, 0], w_r.at[1, 0])
    on_right = remote(w.at[left, 0], w.at[left, 0], w_s.at[4], w_r.at[3, 0], (p, right, t))
    on_right.start()
    arrived(w.at[right, 1], w_r.at[2, 1])
    on_left = remote(w.at[right, 1], w.at[right, 1], w_s.at[5], w_r.at[3, 1], (p, left, t))
    on_left.start()

    def wait_prev(i, _):
        b = lax.rem(p + i, NSP)
        arrived(pv_in.at[b], pv_r.at[b])
        return 0

    lax.fori_loop(1, NSP, wait_prev, 0)

    def cell_out(k, _):
        state = pv_in[:, pl.ds(pl.multiple_of(8 + 8 * k, 8), 8), :].reshape(128, 128)
        high = state.astype(BF16)
        low = (state - high.astype(F32)).astype(BF16)
        before = pv_in[0, pl.ds(k, 1), :]
        for i in range(2):
            h = 2 * k + i
            q = q_half(k, i)
            carried = dot_nt(high, q) + dot_nt(low, q)
            cum_h = cum_s[pl.ds(h, 1), :]
            inside = cum_h + m_s[pl.ds(h, 1), :]
            inter = cum_h + before[:, 64 * i : 64 * i + 1]
            stab = jnp.maximum(inside, inter)
            hidden = jnp.exp(inside - stab) * intra[h] + jnp.exp(inter - stab) * carried
            factor = lax.rsqrt(jnp.mean(hidden * hidden, axis=0, keepdims=True) + EPS)
            actc[:, cols(h)] = jnp.transpose(hidden * factor).astype(BF16)
        return 0

    lax.fori_loop(0, 4, cell_out, 0)

    def wait_attn(j, _):
        here = jnp.logical_and(HEADS * t + j == p, owner == t)

        @pl.when(jnp.logical_not(here))
        def _():
            arrived(acta.at[:, cols(j)], ar.at[j])

        return 0

    lax.fori_loop(0, HEADS, wait_attn, 0)

    def rows_of(core):
        return pl.ds(pl.multiple_of(core * 128, 128), 128)

    for i, block in enumerate((f, left, right, across)):
        for k in range(2):
            if (i, k) not in ((1, 0), (2, 1)):
                arrived(w.at[block, k], w_r.at[i, k])

        def product(core):
            return dot_nn(acta[rows_of(core), :], w[block, 0]) + dot_nn(actc[rows_of(core), :], w[block, 1])

        part[i] = product(1 - t).astype(BF16)
        remote(part.at[i], got.at[i], p_s.at[i], p_r.at[i], (p, f, 1 - t)).start()
        own[i] = product(t).astype(BF16)
    for i, block in enumerate((f, left, right, across)):
        arrived(got.at[i], p_r.at[i])
        total = own[i].astype(F32) + got[i].astype(F32)
        out[:, pl.ds(pl.multiple_of(block * 512, 512), 512)] = total.astype(BF16)

    def drain_heads(j, _):
        here = jnp.logical_and(HEADS * t + j == p, t == owner)

        @pl.when(jnp.logical_not(here))
        def _():
            sent(ak.at[:, cols(j)], k_s.at[j])
            sent(av.at[:, cols(j)], v_s.at[j])
            sent(aq.at[:, cols(j)], q_s.at[j])

        mine = 2 * j + lax.rem(j + t, 2)
        sent(kv_at(kb, mine), rk_s.at[j])
        sent(kv_at(vb, mine), rv_s.at[j])

        @pl.when(jnp.logical_not(jnp.logical_and(mine == p, group == t)))
        def _():
            sent(aout.at[j], as_.at[j])

        return 0

    lax.fori_loop(0, HEADS, drain_heads, 0)

    def drain_states(i, _):
        to = lax.rem(p + i, NSP)
        sent(st_out.at[to], st_s.at[to])
        sent(pv_out.at[to], pv_s.at[to])
        return 0

    lax.fori_loop(1, NSP, drain_states, 0)
    for copy in (*to_right, *to_left, on_right, on_left, lam_copy):
        copy.wait_send()
    for i in range(4):
        sent(part.at[i], p_s.at[i])


def per_device(aq, ak, av, lam, cq, ck, cv, gi, gf, wa, wc):
    dma = pltpu.SemaphoreType.DMA
    scratch = [
        pltpu.VMEM((8, 512, 128), BF16),
        pltpu.VMEM((8, 512, 128), BF16),
        pltpu.VMEM((8, 128, 512), BF16),
        pltpu.VMEM((8, TOK, 128), BF16),
        pltpu.VMEM((2, 8, 512, TOK), F32),
        pltpu.VMEM((2, 8, TOK), F32),
        pltpu.VMEM((2, 8, TOK), F32),
        pltpu.VMEM((2, 128, TOK), F32),
        pltpu.VMEM((8, TOK, 128), BF16),
        pltpu.VMEM((TOK, 1024), BF16),
        pltpu.VMEM((TOK, 1024), BF16),
        pltpu.VMEM((NFS, 2, 1024, 512), BF16),
        pltpu.VMEM((NFS, 128, 512), BF16),
        pltpu.VMEM((NFS, 128, 512), BF16),
        pltpu.VMEM((NFS, 128, 512), BF16),
        pltpu.VMEM((TOK, 512), BF16),
        pltpu.VMEM((TOK, 512), BF16),
        pltpu.VMEM((TOK, 1024), BF16),
        pltpu.VMEM((HEADS, 128, TOK), F32),
        pltpu.VMEM((HEADS, 128, TOK), BF16),
        pltpu.VMEM((8, 128), F32),
        pltpu.VMEM((NSP, 40, 128), F32),
        pltpu.VMEM((NSP, 40, 128), F32),
        pltpu.VMEM((NSP, 40, 128), F32),
        pltpu.VMEM((NSP, 40, 128), F32),
        pltpu.VMEM((HEADS, TOK), F32),
        pltpu.VMEM((HEADS, TOK), F32),
        pltpu.VMEM((HEADS, TOK), F32),
        pltpu.VMEM((2, HEADS, TOK), F32),
        dma((8,)), dma((8,)), dma((8,)),
        dma((16,)), dma((16,)), dma((8,)),
        dma((8,)), dma((8,)),
        dma((8,)), dma((8,)),
        dma((6,)), dma((4, 2)),
        dma((4,)), dma((4,)),
        dma((16,)), dma((16,)), dma((16,)), dma((16,)),
        dma((3,)), dma(()), dma(()),
    ]
    hbm = pl.BlockSpec(memory_space=pl.ANY)
    vmem = pl.BlockSpec(memory_space=pltpu.VMEM)
    smem = pl.BlockSpec(memory_space=pltpu.SMEM)
    y = pl.pallas_call(
        kernel,
        out_shape=jax.ShapeDtypeStruct((128, 2048), BF16),
        in_specs=[hbm, hbm, hbm, smem, hbm, hbm, hbm, vmem, vmem, hbm, hbm],
        out_specs=vmem,
        scratch_shapes=scratch,
        compiler_params=pltpu.CompilerParams(
            collective_id=0, has_side_effects=True, vmem_limit_bytes=56 * 1024 * 1024
        ),
    )(aq[0], ak[0], av[0], lam, cq[0], ck[0], cv[0], gi[0], gf[0], wa, wc)
    return y[None]


def solution(mesh):
    placed = (
        P("fs", "sp", "tp"),
        P("fs", "sp", "tp"),
        P("fs", "sp", "tp"),
        P("tp"),
        P("fs", "sp", "tp"),
        P("fs", "sp", "tp"),
        P("fs", "sp", "tp"),
        P("fs", "tp", "sp"),
        P("fs", "tp", "sp"),
        P("tp", "fs"),
        P("tp", "fs"),
    )
    return jax.shard_map(
        per_device,
        mesh=mesh,
        in_specs=placed,
        out_specs=P("fs", ("sp", "tp"), None),
        check_vma=False,
    )
```

```python
import functools

import jax
import jax.numpy as jnp
from jax import lax
from jax.experimental import pallas as pl
from jax.experimental.pallas import tpu as pltpu
from jax.sharding import PartitionSpec as P

MESH = pl.DeviceIdType.MESH
F32 = jnp.float32
BF16 = jnp.bfloat16
NEG = -1e30
EPS = 1e-6

TOK = 256
NSP = 16
NFS = 4
HEADS = 8
DV = 128


def dot_nn(a, b):
    return jnp.dot(a, b, preferred_element_type=F32)


def dot_nt(a, b):
    return lax.dot_general(a, b, (((1,), (1,)), ((), ())), preferred_element_type=F32)


def iota(shape, dim):
    return lax.broadcasted_iota(jnp.int32, shape, dim)


def log_sigmoid(x):
    small = jnp.exp(-jnp.abs(x))
    series = small * (1.0 - small * (0.5 - small * (1.0 / 3.0 - small * 0.25)))
    return jnp.minimum(x, 0.0) - jnp.where(small < 0.01, series, jnp.log(1.0 + small))


def scan_lanes(x, combine, start):
    lane = iota(x.shape, 1)
    shift = 1
    while shift < x.shape[1]:
        moved = pltpu.roll(x, shift, 1)
        x = combine(x, jnp.where(lane >= shift, moved, start))
        shift *= 2
    return x


def kernel(
    aq, ak, av, lam, cq, ck, cv, gi, gf, wa, wc, out,
    kb, vb, vt, qb, sbuf, mx, ls, acc, aout, acta, actc, w, part, own, got,
    cqs, cks, cvs, intra, cvt, hdr, st_out, st_in, pv_out, pv_in, cum_s, u_s, m_s, lamt,
    k_s, v_s, q_s, k_r, v_r, q_r, rk_s, rv_s, as_, ar, w_s, w_r, p_s, p_r,
    st_s, st_r, pv_s, pv_r, c_r, l_s, l_r, f_s, f_r, b_s, b_r,
):
    p = lax.axis_index("sp")
    f = lax.axis_index("fs")
    t = lax.axis_index("tp")
    left, right, across = lax.rem(f + 3, NFS), lax.rem(f + 1, NFS), lax.rem(f + 2, NFS)
    owner = lax.rem((p + 1) // 2, 2)
    group = p // HEADS
    row = lax.rem(p, HEADS)

    def remote(src, dst, send, recv, device):
        return pltpu.make_async_remote_copy(
            src_ref=src, dst_ref=dst, send_sem=send, recv_sem=recv, device_id=device, device_id_type=MESH
        )

    def arrived(dst, recv):
        remote(dst, dst, recv, recv, (p, f, 1 - t)).wait_recv()

    def sent(src, send):
        remote(src, src, send, send, (p, f, 1 - t)).wait_send()

    def kv_at(ref, b):
        return ref.at[b // 2, pl.ds(pl.multiple_of(lax.rem(b, 2) * TOK, TOK), TOK), :]

    def cols(i):
        return pl.ds(pl.multiple_of(i * 128, 128), 128)

    barrier = pltpu.get_barrier_semaphore()

    def greet(i, _):
        peer = lax.rem(p * 2 + t + i, 2 * NSP)
        pl.semaphore_signal(barrier, inc=1, device_id=(peer // 2, f, lax.rem(peer, 2)), device_id_type=MESH)
        return 0

    with jax.named_scope("barrier"):
        lax.fori_loop(1, 2 * NSP, greet, 0)
        for side in (left, right, across):
            pl.semaphore_signal(barrier, inc=1, device_id=(p, side, t), device_id_type=MESH)
        pl.semaphore_wait(barrier, 2 * NSP + 2)

    locals_ = (
        (cq, cqs, c_r.at[0]), (ck, cks, c_r.at[1]), (cv, cvs, c_r.at[2]),
        (wa, w.at[f, 0], w_r.at[0, 0]), (wc, w.at[f, 1], w_r.at[0, 1]),
    )
    for src, dst, sem in locals_:
        pltpu.make_async_copy(src, dst, sem).start()

    def send_heads(i, _):
        j = lax.rem(row + i, HEADS)
        h = HEADS * t + j
        here = jnp.logical_and(h == p, t == owner)
        trips = (
            (ak, kv_at(kb, p), k_s, k_r.at[p]),
            (av, kv_at(vb, p), v_s, v_r.at[p]),
            (aq, qb.at[p // 2], q_s, q_r.at[p // 2]),
        )
        for src, dst, send, recv in trips:

            @pl.when(jnp.logical_not(here))
            def _():
                remote(src.at[:, cols(j)], dst, send.at[j], recv, (h, f, owner)).start()

            @pl.when(here)
            def _():
                pltpu.make_async_copy(src.at[:, cols(j)], dst, recv).start()

        return 0

    with jax.named_scope("send_heads"):
        lax.fori_loop(0, HEADS, send_heads, 0)

    z, y = p // 4, lax.rem(p, 4)
    pieces = (
        pl.ds(pl.multiple_of(y * 128, 128), 128),
        pl.ds(pl.multiple_of(512 + z * 128, 128), 128),
    )
    first = []
    for i, to in ((1, right), (2, left), (3, across)):
        for k, rows in enumerate(pieces):
            first.append(remote(wa.at[rows], w.at[f, 0, rows], f_s.at[i - 1, k], f_r.at[i - 1, k], (p, to, t)))
    halves = (pl.ds(0, 512), pl.ds(512, 512))
    to_right = [remote(wc.at[rows], w.at[f, 1, rows], w_s.at[k], w_r.at[1, k], (p, right, t)) for k, rows in enumerate(halves)]
    to_left = [remote(wc.at[rows], w.at[f, 1, rows], w_s.at[2 + k], w_r.at[2, k], (p, left, t)) for k, rows in enumerate(halves)]
    for copy in (*first, to_right[0], to_left[1], to_right[1], to_left[0]):
        copy.start()

    def along(axis, d):
        return (z * 4 + lax.rem(y + d, 4), f, t) if axis == 0 else (lax.rem(z + d, 4) * 4 + y, f, t)

    def fan_out(i, block):
        for k, rows in enumerate(pieces):
            piece = w.at[block, 0, rows]
            arrived(piece, f_r.at[i, k])
            for d in (1, 2, 3):
                remote(piece, piece, b_s.at[i, k, d - 1], b_r.at[i, k, (y, z)[k]], along(k, d)).start()

    for i in range(HEADS):
        lamt[t, pl.ds(i, 1), :] = jnp.full((1, TOK), lam[i], F32)
    lam_copy = remote(lamt.at[t], lamt.at[t], l_s, l_r, (p, f, 1 - t))
    lam_copy.start()

    cum = scan_lanes(log_sigmoid(gf[...]), jnp.add, 0.0)
    u = gi[...] - cum
    run = scan_lanes(u, jnp.maximum, NEG)
    cum_s[...] = cum
    u_s[...] = u
    m_s[...] = run
    half = iota((1, 128), 1) < 64
    decay = jnp.broadcast_to(cum[:, TOK - 1 : TOK], (HEADS, 128))
    largest = decay + run[:, TOK - 1 : TOK]
    for k in range(4):
        hdr[k : k + 1, :] = jnp.where(half, decay[2 * k : 2 * k + 1], decay[2 * k + 1 : 2 * k + 2])
        hdr[4 + k : 5 + k, :] = jnp.where(half, largest[2 * k : 2 * k + 1], largest[2 * k + 1 : 2 * k + 2])
    st_out[:, 0:8, :] = jnp.broadcast_to(hdr[...][None], (NSP, 8, 128))
    for src, dst, sem in locals_[:3]:
        pltpu.make_async_copy(src, dst, sem).wait()

    def down(h):
        return jnp.transpose(jnp.broadcast_to(u_s[pl.ds(h, 1), :], (128, TOK)))

    def q_half(pair, which):
        q = cqs[:, cols(pair)] * jnp.asarray(0.125, BF16)
        lane = iota((TOK, 128), 1)
        keep = lane < 64 if which == 0 else lane >= 64
        return jnp.where(keep, q, jnp.zeros_like(q))

    def cell_state(k, _):
        expo = []
        for i in range(2):
            h = 2 * k + i
            expo.append(down(h) - m_s[pl.ds(h, 1), :][:, TOK - 1 : TOK])
            cvt[h] = jnp.transpose(cvs[:, cols(h)].astype(F32)).astype(BF16)
        scaled = jnp.exp(jnp.where(half, expo[0], expo[1]))
        weighted = (scaled * cks[:, cols(k)].astype(F32)).astype(BF16)
        state = jnp.where(half, dot_nn(cvt[2 * k], weighted), dot_nn(cvt[2 * k + 1], weighted))
        st_out[:, pl.ds(pl.multiple_of(8 + 8 * k, 8), 8), :] = state.reshape(NSP, 8, 128)
        return 0

    with jax.named_scope("cell_state"):
        lax.fori_loop(0, 4, cell_state, 0)

    def send_state(i, _):
        to = lax.rem(p + i, NSP)
        remote(st_out.at[to], st_in.at[p], st_s.at[to], st_r.at[p], (to, f, t)).start()
        return 0

    lax.fori_loop(1, NSP, send_state, 0)
    st_in[p] = st_out[p]
    with jax.named_scope("fan_out"):
        fan_out(0, left)
        fan_out(1, right)

    def cell_inside(k, _):
        keys = cks[:, cols(k)]
        causal = iota((TOK, TOK), 0) <= iota((TOK, TOK), 1)
        for i in range(2):
            h = 2 * k + i
            scores = dot_nt(keys, q_half(k, i))
            rows = down(h)
            diff = jnp.concatenate([rows, rows], axis=1) - m_s[pl.ds(h, 1), :]
            weight = (jnp.exp(jnp.where(causal, diff, NEG)) * scores).astype(BF16)
            intra[h] = dot_nn(cvt[h], weight)
        return 0

    with jax.named_scope("cell_inside"):
        lax.fori_loop(0, 4, cell_inside, 0)

    with jax.named_scope("fan_out"):
        fan_out(2, across)

    def scan_states():
        def wait_state(i, _):
            b = lax.rem(p + i, NSP)
            arrived(st_in.at[b], st_r.at[b])
            return 0

        with jax.named_scope("wait_state"):
            lax.fori_loop(1, NSP, wait_state, 0)

        def advance(b, carry):
            stab, states = carry
            pv_out[b, 0:4, :] = stab
            decays, tops = st_in[b, 0:4, :], st_in[b, 4:8, :]
            new = jnp.maximum(decays + stab, tops)
            keep, take = jnp.exp(decays + stab - new), jnp.exp(tops - new)
            after = []
            for k in range(4):
                at = slice(8 + 8 * k, 16 + 8 * k)
                pv_out[b, at, :] = states[k]
                after.append(keep[k : k + 1] * states[k] + take[k : k + 1] * st_in[b, at, :])
            return new, tuple(after)

        zero = jnp.zeros((8, 128), F32)
        pv_out[:, 4:8, :] = jnp.zeros((NSP, 4, 128), F32)
        with jax.named_scope("advance"):
            lax.fori_loop(0, NSP, advance, (jnp.zeros((4, 128), F32), (zero,) * 4))

        def send_prev(i, _):
            to = lax.rem(p + i, NSP)
            remote(pv_out.at[to], pv_in.at[p], pv_s.at[to], pv_r.at[p], (to, f, t)).start()
            return 0

        lax.fori_loop(1, NSP, send_prev, 0)
        pv_in[p] = pv_out[p]

    on_right = remote(w.at[left, 1, halves[0]], w.at[left, 1, halves[0]], w_s.at[4], w_r.at[3, 0], (p, right, t))
    on_left = remote(w.at[right, 1, halves[1]], w.at[right, 1, halves[1]], w_s.at[5], w_r.at[3, 1], (p, left, t))

    def forward():
        with jax.named_scope("wait_ring"):
            arrived(w.at[left, 1, halves[0]], w_r.at[1, 0])
        on_right.start()
        with jax.named_scope("wait_ring"):
            arrived(w.at[right, 1, halves[1]], w_r.at[2, 1])
        on_left.start()

    def pass_on(s):
        mine = 2 * s + lax.rem(s + t, 2)
        for ref, recv, send in ((kb, k_r, rk_s), (vb, v_r, rv_s)):
            block = kv_at(ref, mine)
            with jax.named_scope("wait_mine"):
                arrived(block, recv.at[mine])
            remote(block, block, send.at[s], recv.at[mine], (p, f, 1 - t)).start()

    arrived(lamt.at[1 - t], l_r)

    def attend(s, _):
        mine = 2 * s + lax.rem(s + t, 2)
        other = 2 * s + lax.rem(s + t + 1, 2)

        @pl.when(s + 2 < HEADS)
        def _():
            pass_on(s + 2)

        pl.when(s == 4)(scan_states)
        pl.when(s == 5)(forward)
        with jax.named_scope("wait_other"):
            arrived(qb.at[s], q_r.at[s])
            for ref, recv in ((kb, k_r), (vb, v_r)):
                arrived(kv_at(ref, other), recv.at[other])
        vt[s] = jnp.transpose(vb[s].astype(F32)).astype(BF16)
        q = qb[s] * jnp.asarray(0.125, BF16)
        lane = iota((TOK, 128), 1)
        none = jnp.zeros_like(q)
        maps = (jnp.where(lane < 64, q, none), jnp.where(lane >= 64, q, none))
        mx[...] = jnp.full(mx.shape, NEG, F32)

        def score(kt, masked):
            keys = kb[kt]
            for c in range(2):
                sc = dot_nt(keys, maps[c])
                if masked:
                    seen = iota(sc.shape, 0) <= iota(sc.shape, 1) + (mine - 2 * s) * TOK
                    sc = jnp.where(seen, sc, NEG)
                sbuf[c, kt] = sc
                mx[c] = jnp.maximum(mx[c], jnp.max(sc.reshape(64, 8, TOK), axis=0))

        def score_one(kt, _):
            score(kt, False)
            return 0

        with jax.named_scope("score"):
            lax.fori_loop(0, s, score_one, 0)
            score(s, True)
        tops = [jnp.max(mx[c], axis=0, keepdims=True) for c in range(2)]
        ls[...] = jnp.zeros(ls.shape, F32)
        acc[...] = jnp.zeros(acc.shape, F32)

        def weigh(kt, _):
            for c in range(2):
                expd = jnp.exp(sbuf[c, kt] - tops[c])
                ls[c] += jnp.sum(expd.reshape(64, 8, TOK), axis=0)
                acc[c] += dot_nn(vt[kt], expd.astype(BF16))
            return 0

        with jax.named_scope("weigh"):
            lax.fori_loop(0, s + 1, weigh, 0)
        ratio = [acc[c] / jnp.sum(ls[c], axis=0, keepdims=True) for c in range(2)]
        mixed = ratio[0] - lamt[group, pl.ds(row, 1), :] * ratio[1]
        factor = lax.rsqrt(jnp.mean(mixed * mixed, axis=0, keepdims=True) + EPS) * 0.8
        aout[s] = jnp.transpose(mixed * factor).astype(BF16)
        home = jnp.logical_and(mine == p, group == t)

        @pl.when(jnp.logical_not(home))
        def _():
            remote(aout.at[s], acta.at[:, cols(row)], as_.at[s], ar.at[row], (mine, f, group)).start()

        @pl.when(home)
        def _():
            acta[:, cols(row)] = aout[s]

        return 0

    pass_on(0)
    pass_on(1)
    with jax.named_scope("attend"):
        lax.fori_loop(0, HEADS, attend, 0)

    def wait_prev(i, _):
        b = lax.rem(p + i, NSP)
        arrived(pv_in.at[b], pv_r.at[b])
        return 0

    with jax.named_scope("wait_prev"):
        lax.fori_loop(1, NSP, wait_prev, 0)

    def cell_out(k, _):
        state = pv_in[:, pl.ds(pl.multiple_of(8 + 8 * k, 8), 8), :].reshape(128, 128)
        high = state.astype(BF16)
        low = (state - high.astype(F32)).astype(BF16)
        before = pv_in[0, pl.ds(k, 1), :]
        for i in range(2):
            h = 2 * k + i
            q = q_half(k, i)
            carried = dot_nt(high, q) + dot_nt(low, q)
            cum_h = cum_s[pl.ds(h, 1), :]
            inside = cum_h + m_s[pl.ds(h, 1), :]
            inter = cum_h + before[:, 64 * i : 64 * i + 1]
            stab = jnp.maximum(inside, inter)
            hidden = jnp.exp(inside - stab) * intra[h] + jnp.exp(inter - stab) * carried
            factor = lax.rsqrt(jnp.mean(hidden * hidden, axis=0, keepdims=True) + EPS)
            actc[:, cols(h)] = jnp.transpose(hidden * factor).astype(BF16)
        return 0

    with jax.named_scope("cell_out"):
        lax.fori_loop(0, 4, cell_out, 0)

    def wait_attn(j, _):
        here = jnp.logical_and(HEADS * t + j == p, owner == t)

        @pl.when(jnp.logical_not(here))
        def _():
            arrived(acta.at[:, cols(j)], ar.at[j])

        return 0

    with jax.named_scope("wait_attn"):
        lax.fori_loop(0, HEADS, wait_attn, 0)

    def rows_of(core):
        return pl.ds(pl.multiple_of(core * 128, 128), 128)

    for i, block in enumerate((f, left, right, across)):
        with jax.named_scope("wait_rows"):
            if i == 0:
                arrived(w.at[block, 0], w_r.at[0, 0])
                arrived(w.at[block, 1], w_r.at[0, 1])
            else:
                for k in range(2):
                    if (i, k) not in ((1, 0), (2, 1)):
                        arrived(w.at[block, 1, halves[k]], w_r.at[i, k])
                for k, own_at in enumerate((y, z)):
                    for d in (1, 2, 3):
                        at = lax.rem(own_at + d, 4)
                        rows = pl.ds(pl.multiple_of(512 * k + at * 128, 128), 128)
                        arrived(w.at[block, 0, rows], b_r.at[i - 1, k, at])

        def product(core):
            return dot_nn(acta[rows_of(core), :], w[block, 0]) + dot_nn(actc[rows_of(core), :], w[block, 1])

        part[i] = product(1 - t).astype(BF16)
        remote(part.at[i], got.at[i], p_s.at[i], p_r.at[i], (p, f, 1 - t)).start()
        own[i] = product(t).astype(BF16)
    for i, block in enumerate((f, left, right, across)):
        with jax.named_scope("wait_got"):
            arrived(got.at[i], p_r.at[i])
        total = own[i].astype(F32) + got[i].astype(F32)
        out[:, pl.ds(pl.multiple_of(block * 512, 512), 512)] = total.astype(BF16)

    def drain_heads(j, _):
        here = jnp.logical_and(HEADS * t + j == p, t == owner)

        @pl.when(jnp.logical_not(here))
        def _():
            sent(ak.at[:, cols(j)], k_s.at[j])
            sent(av.at[:, cols(j)], v_s.at[j])
            sent(aq.at[:, cols(j)], q_s.at[j])

        mine = 2 * j + lax.rem(j + t, 2)
        sent(kv_at(kb, mine), rk_s.at[j])
        sent(kv_at(vb, mine), rv_s.at[j])

        @pl.when(jnp.logical_not(jnp.logical_and(mine == p, group == t)))
        def _():
            sent(aout.at[j], as_.at[j])

        return 0

    with jax.named_scope("drain"):
        lax.fori_loop(0, HEADS, drain_heads, 0)

    def drain_states(i, _):
        to = lax.rem(p + i, NSP)
        sent(st_out.at[to], st_s.at[to])
        sent(pv_out.at[to], pv_s.at[to])
        return 0

    lax.fori_loop(1, NSP, drain_states, 0)
    for copy in (*first, *to_right, *to_left, on_right, on_left, lam_copy):
        copy.wait_send()
    for i, block in enumerate((left, right, across)):
        for k, rows in enumerate(pieces):
            for d in range(3):
                sent(w.at[block, 0, rows], b_s.at[i, k, d])
    for i in range(4):
        sent(part.at[i], p_s.at[i])


def per_device(aq, ak, av, lam, cq, ck, cv, gi, gf, wa, wc):
    dma = pltpu.SemaphoreType.DMA
    scratch = [
        pltpu.VMEM((8, 512, 128), BF16),
        pltpu.VMEM((8, 512, 128), BF16),
        pltpu.VMEM((8, 128, 512), BF16),
        pltpu.VMEM((8, TOK, 128), BF16),
        pltpu.VMEM((2, 8, 512, TOK), F32),
        pltpu.VMEM((2, 8, TOK), F32),
        pltpu.VMEM((2, 8, TOK), F32),
        pltpu.VMEM((2, 128, TOK), F32),
        pltpu.VMEM((8, TOK, 128), BF16),
        pltpu.VMEM((TOK, 1024), BF16),
        pltpu.VMEM((TOK, 1024), BF16),
        pltpu.VMEM((NFS, 2, 1024, 512), BF16),
        pltpu.VMEM((NFS, 128, 512), BF16),
        pltpu.VMEM((NFS, 128, 512), BF16),
        pltpu.VMEM((NFS, 128, 512), BF16),
        pltpu.VMEM((TOK, 512), BF16),
        pltpu.VMEM((TOK, 512), BF16),
        pltpu.VMEM((TOK, 1024), BF16),
        pltpu.VMEM((HEADS, 128, TOK), F32),
        pltpu.VMEM((HEADS, 128, TOK), BF16),
        pltpu.VMEM((8, 128), F32),
        pltpu.VMEM((NSP, 40, 128), F32),
        pltpu.VMEM((NSP, 40, 128), F32),
        pltpu.VMEM((NSP, 40, 128), F32),
        pltpu.VMEM((NSP, 40, 128), F32),
        pltpu.VMEM((HEADS, TOK), F32),
        pltpu.VMEM((HEADS, TOK), F32),
        pltpu.VMEM((HEADS, TOK), F32),
        pltpu.VMEM((2, HEADS, TOK), F32),
        dma((8,)), dma((8,)), dma((8,)),
        dma((16,)), dma((16,)), dma((8,)),
        dma((8,)), dma((8,)),
        dma((8,)), dma((8,)),
        dma((6,)), dma((4, 2)),
        dma((4,)), dma((4,)),
        dma((16,)), dma((16,)), dma((16,)), dma((16,)),
        dma((3,)), dma(()), dma(()),
        dma((3, 2)), dma((3, 2)), dma((3, 2, 3)), dma((3, 2, 4)),
    ]
    hbm = pl.BlockSpec(memory_space=pl.ANY)
    vmem = pl.BlockSpec(memory_space=pltpu.VMEM)
    smem = pl.BlockSpec(memory_space=pltpu.SMEM)
    y = pl.pallas_call(
        kernel,
        out_shape=jax.ShapeDtypeStruct((128, 2048), BF16),
        in_specs=[hbm, hbm, hbm, smem, hbm, hbm, hbm, vmem, vmem, hbm, hbm],
        out_specs=vmem,
        scratch_shapes=scratch,
        compiler_params=pltpu.CompilerParams(
            collective_id=0, has_side_effects=True, vmem_limit_bytes=56 * 1024 * 1024
        ),
    )(aq[0], ak[0], av[0], lam, cq[0], ck[0], cv[0], gi[0], gf[0], wa, wc)
    return y[None]


def solution(mesh):
    placed = (
        P("fs", "sp", "tp"),
        P("fs", "sp", "tp"),
        P("fs", "sp", "tp"),
        P("tp"),
        P("fs", "sp", "tp"),
        P("fs", "sp", "tp"),
        P("fs", "sp", "tp"),
        P("fs", "tp", "sp"),
        P("fs", "tp", "sp"),
        P("tp", "fs"),
        P("tp", "fs"),
    )
    return jax.shard_map(
        per_device,
        mesh=mesh,
        in_specs=placed,
        out_specs=P("fs", ("sp", "tp"), None),
        check_vma=False,
    )
```
